32 devices in a mesh: ep: 8 (over z, core), tp: 4 (over y, x).
Axes of the slice: x: 2, y: 2, z: 4, core: 2. Of those that a mesh axis runs over, the one named last changes fastest.
Arguments:
- tokens: bfloat16 [1536, 2048], P('ep'), may hold values from -6 to 6
- moe_out: bfloat16 [1536, 2048], P('ep', 'tp'), may hold values from -16 to 16
- out_grad: bfloat16 [1536, 2048], P('ep', 'tp'), may hold values from -3 to 3
- norm_gain: float32 [2048], P('tp'), may hold values from 0.1 to 1.9
- gate_weights: bfloat16 [1536, 2], P('ep'), may hold values from 0.099609375 to 1
- expert_ids: int32 [1536, 2], P('ep'), may hold values from 0 to 7, as said below
- gate_w: bfloat16 [8, 1536, 2048], P('ep', 'tp'), may hold values from -0.125 to 0.125
- up_w: bfloat16 [8, 1536, 2048], P('ep', 'tp'), may hold values from -0.125 to 0.125
- down_w: bfloat16 [8, 1536, 2048], P('ep', 'tp'), may hold values from -0.15625 to 0.15625
Outputs:
- token_grad: bfloat16 [1536, 2048], P('ep', 'tp')
- gate_grad: bfloat16 [1536, 2], P('ep')
- gate_w_grad: float32 [8, 1536, 2048], P('ep', 'tp')
- up_w_grad: float32 [8, 1536, 2048], P('ep', 'tp')
- down_w_grad: float32 [8, 1536, 2048], P('ep', 'tp')
The draws below stay inside these ranges and needn't reach their ends.
Inputs may be any that keep to these rules, and one draw needn't show every extreme that they name: `expert_ids`: each row names 2 different experts of one group, ids g * 2 to g * 2 + 1. In each aligned block of 192 rows (the rows of one device) no expert is named more than 96 times, and in every draw all experts of one group are named exactly 96 times in every block.
All inputs are finite; a program needn't handle non-finite values.
Results may differ from the reference program's by a relative error of at most 0.015.
Values may be sent and summed in bfloat16 or wider, within the bound.
A program may use at most 64 MiB of HBM per device.

```python
import math
import jax
import jax.numpy as jnp
from jax import lax

D = 2048
D_EXPERT = 1536
TOK_DEV = 192
TOPK = 2
GROUPS = 4
EXPERTS = 8
EXP_GROUP = 2
CAP = 96
F_DEV = 384
TOKENS = 1536
N_EP = 8
N_TP = 4


def draw_moe_out(key, part):
    first, second, third, fourth = jax.random.split(jax.random.fold_in(key, 11), 4)
    base = jax.random.normal(first, (TOKENS, D), jnp.float32)
    group_scale = jnp.exp(jax.random.uniform(second, (32,), jnp.float32, math.log(0.2), math.log(4.0)))
    column_scale = jnp.repeat(group_scale, D // 32)
    values = jnp.clip(base * column_scale[None, :], -16.0, 16.0)
    return values.astype(jnp.bfloat16)


def draw_expert_ids(key, part):
    blocks = TOKENS // TOK_DEV
    n_full = 2 * TOK_DEV // GROUPS
    key_full, key_blocks = jax.random.split(jax.random.fold_in(key, 7))
    full_group = jax.random.randint(key_full, (), 0, GROUPS)

    def one_block(block_key):
        first, second, third = jax.random.split(block_key, 3)
        order = jax.random.permutation(first, TOK_DEV)
        places = jnp.arange(TOK_DEV)
        others = (full_group + 1 + jax.random.randint(second, (TOK_DEV,), 0, GROUPS - 1)) % GROUPS
        group = jnp.where(places < n_full, full_group, others).astype(jnp.int32)
        member = (group[:, None] == jnp.arange(GROUPS, dtype=jnp.int32)[None, :]).astype(jnp.int32)
        ranks = jnp.sum((jnp.cumsum(member, axis=0) - member) * member, axis=1)
        shuffles = jax.vmap(lambda sub_key: jax.random.permutation(sub_key, EXP_GROUP))(jax.random.split(third, GROUPS))
        within = (ranks[:, None] * TOPK + jnp.arange(TOPK)[None, :]) % EXP_GROUP
        local = shuffles[group[:, None], within]
        chosen = (group[:, None] * EXP_GROUP + local).astype(jnp.int32)
        return jnp.zeros((TOK_DEV, TOPK), jnp.int32).at[order].set(chosen)
    identity = jax.vmap(one_block)(jax.random.split(key_blocks, blocks))
    return identity.reshape(TOKENS, TOPK).astype(jnp.int32)


def steps_of(own_key, dims, pieces, least, largest):
    def one(axis_at, parts):
        heights = jax.random.uniform(jax.random.fold_in(jax.random.fold_in(own_key, 6), axis_at), (parts,), jnp.float32, least / len(pieces), largest / len(pieces))
        return jnp.repeat(jnp.exp(heights), dims[axis_at] // parts).reshape((-1,) + (1,) * (len(dims) - axis_at - 1))

    factor_of = one(*pieces[0])
    for cut in pieces[1:]:
        factor_of = factor_of * one(*cut)
    return factor_of


def centred(rng, dims, scale, most, shards=(), held_as=jnp.bfloat16):
    entries = scale * jax.random.normal(rng, dims, jnp.float32)
    if shards:
        entries = entries * steps_of(rng, dims, shards, -0.22, 0.18)
    return jnp.clip(entries, -most, most).astype(held_as)


def setup_inputs(seed: int = 0) -> dict:
    keys = jax.random.split(jax.random.key(seed), 10)
    tokens = centred(keys[0], (TOKENS, D), 1.0, 6.0, ((0, 8),))
    moe_out = draw_moe_out(jax.random.fold_in(keys[9], 71), 0)
    out_grad = centred(keys[2], (TOKENS, D), 0.5, 3.0, ((0, 8), (1, 4)))
    norm_gain = jnp.clip(1.0 + 0.18 * jax.random.normal(keys[3], (D,), jnp.float32), 0.1, 1.9)
    gate_weights = jnp.clip(0.099609375 + 0.9003906 * jax.random.uniform(keys[4], (TOKENS, TOPK), jnp.float32) ** steps_of(keys[4], (TOKENS, TOPK), ((0, 8),), -0.2, 0.2), 0.099609375, 1.0).astype(jnp.bfloat16)
    expert_ids = draw_expert_ids(jax.random.fold_in(keys[9], 71), 0)
    gate_w = centred(keys[6], (EXPERTS, D_EXPERT, D), D ** -0.5, 0.125, ((0, 8), (1, 4)))
    up_w = centred(keys[7], (EXPERTS, D_EXPERT, D), D ** -0.5, 0.125, ((0, 8), (1, 4)))
    down_w = centred(keys[8], (EXPERTS, D_EXPERT, D), D_EXPERT ** -0.5, 0.15625, ((0, 8), (1, 4)))
    return dict(tokens=tokens, moe_out=moe_out, out_grad=out_grad, norm_gain=norm_gain, gate_weights=gate_weights, expert_ids=expert_ids, gate_w=gate_w, up_w=up_w, down_w=down_w)


EPSILON = 0.25

def reference(tokens, moe_out, out_grad, norm_gain, gate_weights, expert_ids, gate_w, up_w, down_w):
    mixed = moe_out.astype(jnp.float32)
    scaled_grad = out_grad.astype(jnp.float32) * norm_gain
    inverse = lax.rsqrt(lax.optimization_barrier(jnp.mean(mixed * mixed, axis=1)) + EPSILON)
    coupling = inverse ** 3 * lax.optimization_barrier(jnp.mean(scaled_grad * mixed, axis=1))
    mix_grad = (inverse[:, None] * scaled_grad - mixed * coupling[:, None]).astype(jnp.bfloat16)
    per_source = expert_ids.reshape(N_EP, TOK_DEV * TOPK)
    one_hot = (per_source[:, :, None] == jnp.arange(EXPERTS, dtype=jnp.int32)[None, None, :]).astype(jnp.int32)
    before = lax.optimization_barrier(jnp.sum((jnp.cumsum(one_hot, axis=1) - one_hot) * one_hot, axis=2))
    source = jnp.arange(N_EP, dtype=jnp.int32)[:, None]
    global_slot = (per_source * (N_EP * CAP) + source * CAP + before).reshape(-1).astype(jnp.int32)
    n_assign = TOKENS * TOPK
    table = jnp.full((EXPERTS * N_EP * CAP,), n_assign, jnp.int32)
    table = table.at[global_slot].set(jnp.arange(n_assign, dtype=jnp.int32)).reshape(EXPERTS, N_EP * CAP)
    token_pad = jnp.concatenate([tokens, jnp.zeros((1, D), jnp.bfloat16)], axis=0)
    grad_pad = jnp.concatenate([mix_grad, jnp.zeros((1, D), jnp.bfloat16)], axis=0)
    weight_pad = jnp.concatenate([gate_weights.reshape(-1).astype(jnp.float32), jnp.zeros((1,), jnp.float32)])

    def expert_pass(packed):
        slots, w_gate, w_up, w_down = packed
        row_index = slots // TOPK
        inputs = token_pad[row_index]
        cotangent = grad_pad[row_index]
        scales = weight_pad[slots][:, None]
        gate_pre = jnp.dot(inputs, w_gate.T, preferred_element_type=jnp.float32)
        up_pre = jnp.dot(inputs, w_up.T, preferred_element_type=jnp.float32)
        hidden_grad = jnp.dot(cotangent, w_down.T, preferred_element_type=jnp.float32)
        sigmoid = jax.nn.sigmoid(gate_pre)
        activated = gate_pre * sigmoid
        gate_total = lax.optimization_barrier(jnp.sum(activated * up_pre * hidden_grad, axis=1)).astype(jnp.bfloat16)
        scaled_hidden = (scales * activated * up_pre).astype(jnp.bfloat16)
        down_grad = jnp.dot(scaled_hidden.T, cotangent, preferred_element_type=jnp.float32)
        gate_delta = (scales * hidden_grad * up_pre * sigmoid * (1.0 + gate_pre * (1.0 - sigmoid))).astype(jnp.bfloat16)
        up_delta = (scales * hidden_grad * activated).astype(jnp.bfloat16)
        gate_grad_w = jnp.dot(gate_delta.T, inputs, preferred_element_type=jnp.float32)
        up_grad_w = jnp.dot(up_delta.T, inputs, preferred_element_type=jnp.float32)
        partial_value = jnp.einsum('rbf,bfd->brd', gate_delta.astype(jnp.float32).reshape(-1, N_TP, F_DEV), w_gate.astype(jnp.float32).reshape(N_TP, F_DEV, D))
        partial_value = partial_value + jnp.einsum('rbf,bfd->brd', up_delta.astype(jnp.float32).reshape(-1, N_TP, F_DEV), w_up.astype(jnp.float32).reshape(N_TP, F_DEV, D))
        rounded = lax.optimization_barrier(partial_value.astype(jnp.bfloat16))
        slot_grad = lax.optimization_barrier(jnp.sum(rounded.astype(jnp.float32), axis=0)).astype(jnp.bfloat16)
        return (gate_grad_w, up_grad_w, down_grad, slot_grad, gate_total)
    results = lax.map(expert_pass, (table, gate_w, up_w, down_w))
    slot_grads = results[3].reshape(-1, D)
    gate_totals = results[4].reshape(-1)
    token_grad = lax.optimization_barrier(jnp.sum(slot_grads[global_slot].reshape(TOKENS, TOPK, D).astype(jnp.float32), axis=1)).astype(jnp.bfloat16)
    gate_grad = gate_totals[global_slot].reshape(TOKENS, TOPK)
    return (token_grad, gate_grad, results[0], results[1], results[2])
```

```python
import functools

import jax
import jax.numpy as jnp
from jax import lax
from jax.experimental import pallas as pl
from jax.experimental.pallas import tpu as pltpu
from jax.sharding import PartitionSpec as P

EPSILON = 0.25
GROUPS = 4
CORES = 2
LANES = 128
MESH = pl.DeviceIdType.MESH
VMEM_SPEC = pl.BlockSpec(memory_space=pltpu.VMEM)
F32 = jnp.float32
BF16 = jnp.bfloat16


def places(zs):
    ep = lax.axis_index("ep")
    tp = lax.axis_index("tp")
    z = ep // CORES
    core = ep % CORES
    near_x = tp + 1 - 2 * (tp % 2)
    near_y = (tp + 2) % 4
    diag = (near_x + 2) % 4
    return ep, tp, z, core, near_x, near_y, diag


def greet(zs):
    ep, tp, z, core, near_x, near_y, diag = places(zs)
    barrier = pltpu.get_barrier_semaphore()
    peers = [(z * CORES + 1 - core, tp), (ep, near_x), (ep, near_y), (ep, diag)]
    peers += [(((z + k) % zs) * CORES + core, tp) for k in range(1, zs)]
    for peer in peers:
        pl.semaphore_signal(barrier, inc=1, device_id=peer, device_id_type=MESH)
    pl.semaphore_wait(barrier, len(peers))


class Sender:
    def __init__(self, send_sem):
        self.send_sem, self.started = send_sem, []

    def __call__(self, src, dst, recv_sem, device):
        copy = pltpu.make_async_remote_copy(
            src_ref=src,
            dst_ref=dst,
            send_sem=self.send_sem.at[len(self.started)],
            recv_sem=recv_sem,
            device_id=device,
            device_id_type=MESH,
        )
        copy.start()
        self.started.append(copy)
        return copy

    def finish(self):
        for copy in self.started:
            copy.wait_send()


def dispatch_kernel(
    zs, cap, width,
    tok_ref, moe_ref, grad_ref, gain_ref, perm_ref, wmat_ref,
    x_ref, g_ref, w_ref,
    pack_x, pack_g, pack_w, stats,
    send_sem, stat_sem, z_sem, w_sem, wp_sem, tp_sem, pair_sem,
):
    ep, tp, z, core, near_x, near_y, diag = places(zs)
    n_tok, full = tok_ref.shape
    partner = (z * CORES + 1 - core, tp)
    send = Sender(send_sem)

    def cols(at):
        return pl.ds(pl.multiple_of(at * width, width), width)

    def rows(source, who=None):
        start = (source * CORES + (core if who is None else who)) * cap
        return pl.ds(pl.multiple_of(start, 16), cap)

    def chip_rows(q):
        return pl.ds(pl.multiple_of(q * cap, 16), cap)

    mixed = moe_ref[...].astype(F32)
    scaled = grad_ref[...].astype(F32) * gain_ref[...]
    squares = jnp.sum(mixed * mixed, axis=1, keepdims=True)
    crossed = jnp.sum(scaled * mixed, axis=1, keepdims=True)
    lane = lax.broadcasted_iota(jnp.int32, (n_tok, LANES), 1)
    both = jnp.where(lane == 0, squares, jnp.where(lane == 1, crossed, 0.0))
    tall = stats.shape[2]
    both = jnp.concatenate([both, jnp.zeros((tall - n_tok, LANES), F32)], axis=0)
    stats[0] = both.T[:8]
    greet(zs)
    got_stats = [
        send(stats.at[0], stats.at[1 + i], stat_sem.at[i], (ep, to))
        for i, to in enumerate((near_x, near_y, diag))
    ]

    tok = tok_ref[:, cols(tp)]
    perm = perm_ref[...]
    pack_x[...] = jnp.dot(perm, tok, preferred_element_type=F32).astype(BF16)
    pack_w[...] = jnp.dot(perm, wmat_ref[...], preferred_element_type=F32).astype(BF16)
    x_ref[rows(z), cols(tp)] = pack_x[chip_rows(z), :]
    w_ref[rows(z), :] = pack_w[chip_rows(z), :]
    outs, packs = (x_ref, g_ref), (pack_x, pack_g)
    z_copies, w_copies = {}, {}

    def z_out(t):
        for k in range(1, zs):
            q = (z + k) % zs
            z_copies[t, k] = send(
                packs[t].at[chip_rows(q)],
                outs[t].at[rows(z), cols(tp)],
                z_sem.at[t, k],
                (q * CORES + core, tp),
            )

    z_out(0)
    for k in range(1, zs):
        q = (z + k) % zs
        w_copies[k] = send(
            pack_w.at[chip_rows(q)], w_ref.at[rows(z)], w_sem.at[k], (q * CORES + core, tp)
        )

    tp_copies, pair_copies = {}, []

    def to_pair(t, k, origin, at):
        block = outs[t].at[rows((z - k + zs) % zs), cols(at)]
        pair_copies.append(send(block, block, pair_sem.at[t, k, origin], partner))

    def arrive(t, k):
        if k:
            z_copies[t, k].wait_recv()
        block = outs[t].at[rows((z - k + zs) % zs), cols(tp)]
        tp_copies[t, k, 0] = send(block, block, tp_sem.at[t, k, 0], (ep, near_x))
        tp_copies[t, k, 1] = send(block, block, tp_sem.at[t, k, 1], (ep, near_y))
        to_pair(t, k, 0, tp)

    def relay(t, k):
        tp_copies[t, k, 0].wait_recv()
        tp_copies[t, k, 1].wait_recv()
        at, to = ((near_x, near_y), (near_y, near_x))[t]
        block = outs[t].at[rows((z - k + zs) % zs), cols(at)]
        tp_copies[t, k, 2] = send(block, block, tp_sem.at[t, k, 2], (ep, to))
        to_pair(t, k, 1, near_x)
        to_pair(t, k, 2, near_y)

    arrive(0, 0)
    for copy in got_stats:
        copy.wait_recv()
    total = stats[0] + stats[1] + stats[2] + stats[3]
    total = jnp.concatenate([total, jnp.zeros((LANES - 8, tall), F32)], axis=0).T[:n_tok]
    inverse = lax.rsqrt(total[:, 0:1] / full + EPSILON)
    coupling = inverse * inverse * inverse * (total[:, 1:2] / full)
    mix = (inverse * scaled - mixed * coupling).astype(BF16)
    pack_g[...] = jnp.dot(perm, mix, preferred_element_type=F32).astype(BF16)
    g_ref[rows(z), cols(tp)] = pack_g[chip_rows(z), :]
    z_out(1)
    arrive(1, 0)

    pair_w = [send(w_ref.at[rows(z)], w_ref.at[rows(z)], wp_sem.at[0], partner)]
    for k in range(1, zs):
        for t in range(2):
            arrive(t, k)
            relay(t, k - 1)
        w_copies[k].wait_recv()
        block = w_ref.at[rows((z - k + zs) % zs)]
        pair_w.append(send(block, block, wp_sem.at[k], partner))
    for t in range(2):
        relay(t, zs - 1)
    for k in range(zs):
        for t in range(2):
            tp_copies[t, k, 2].wait_recv()
            to_pair(t, k, 3, diag)
    for copy in pair_w + pair_copies:
        copy.wait_recv()
    send.finish()


def return_kernel(
    zs, cap, width,
    part_ref, gate_ref,
    back_ref, total_ref,
    comb, pin, first_in, second_out, second_in, final, gates,
    send_sem, pin_sem, one_sem, two_sem, z_sem, gate_sem, gz_sem,
):
    ep, tp, z, core, near_x, near_y, diag = places(zs)
    partner = (z * CORES + 1 - core, tp)
    send = Sender(send_sem)
    half = width // 2
    order = list(range(1, zs)) + [0]

    def rows(source, who):
        return pl.ds(pl.multiple_of((source * CORES + who) * cap, 16), cap)

    def chip_rows(q):
        return pl.ds(pl.multiple_of(q * cap, 16), cap)

    def cols(at, which):
        return pl.ds(pl.multiple_of(at * width + which * half, half), half)

    gates[0, core] = gate_ref[...]
    greet(zs)
    pin_copies, one, two, back = {}, {}, {}, {}
    pair_gate = send(gate_ref, gates.at[0, core], gate_sem.at[3], partner)
    for k in order:
        q = (z + k) % zs
        pin_copies[k] = send(
            part_ref.at[rows(q, 1 - core)], pin.at[k], pin_sem.at[k], partner
        )
    pair_gate.wait_recv()
    gate_copies = [
        send(gates.at[0], gates.at[1 + i], gate_sem.at[i], (ep, to))
        for i, to in enumerate((near_x, near_y, diag))
    ]

    def stage_one(k):
        q = (z + k) % zs
        pin_copies[k].wait_recv()
        comb[k] = (part_ref[rows(q, core), :].astype(F32) + pin[k].astype(F32)).astype(BF16)
        for which, near in enumerate((near_x, near_y)):
            for i, at in enumerate((near, diag)):
                one[k, which, i] = send(
                    comb.at[k, :, cols(at, which)],
                    first_in.at[k, which, i],
                    one_sem.at[k, which, i],
                    (ep, near),
                )

    def stage_two(k):
        for which, far in enumerate((near_y, near_x)):
            one[k, which, 1].wait_recv()
            second_out[k, which] = (
                comb[k, :, cols(far, which)].astype(F32) + first_in[k, which, 1].astype(F32)
            ).astype(BF16)
            two[k, which] = send(
                second_out.at[k, which], second_in.at[k, which], two_sem.at[k, which], (ep, far)
            )

    def stage_three(k):
        q = (z + k) % zs
        for which in range(2):
            one[k, which, 0].wait_recv()
            two[k, which].wait_recv()
            final[k, :, which * half : (which + 1) * half] = (
                comb[k, :, cols(tp, which)].astype(F32)
                + first_in[k, which, 0].astype(F32)
                + second_in[k, which].astype(F32)
            ).astype(BF16)
        if k:
            back[k] = send(
                final.at[k], back_ref.at[chip_rows(z)], z_sem.at[k], (q * CORES + core, tp)
            )
        else:
            back_ref[chip_rows(z), :] = final[0]

    for k in order:
        stage_one(k)
    for copy in gate_copies:
        copy.wait_recv()
    total_ref[z] = gates[0] + gates[1] + gates[2] + gates[3]
    gate_back = [
        send(total_ref.at[z], total_ref.at[z], gz_sem.at[k], (((z + k) % zs) * CORES + core, tp))
        for k in range(1, zs)
    ]
    for at, k in enumerate(order):
        stage_two(k)
        if at:
            stage_three(order[at - 1])
    stage_three(order[-1])
    for copy in list(back.values()) + gate_back:
        copy.wait_recv()
    send.finish()


def pick_rows(matrix, slot_token, n_experts, capacity):
    padded = jnp.concatenate([matrix, jnp.zeros((1, matrix.shape[1]), matrix.dtype)], axis=0)
    return padded[slot_token].reshape(n_experts, capacity, matrix.shape[1])


def general(tokens, moe_out, out_grad, norm_gain, gate_weights, expert_ids, gate_w, up_w, down_w):
    tok_count = tokens.shape[0]
    full_width = tokens.shape[1]
    col_width = moe_out.shape[1]
    ep_count = lax.axis_size("ep")
    exp_local = gate_w.shape[0]
    n_experts = ep_count * exp_local
    top_count = expert_ids.shape[1]
    capacity = 2 * tok_count * top_count // n_experts
    mixed = moe_out.astype(jnp.float32)
    scaled_grad = out_grad.astype(jnp.float32) * norm_gain
    squares, crossed = lax.psum(
        (jnp.sum(mixed * mixed, axis=1), jnp.sum(scaled_grad * mixed, axis=1)), "tp"
    )
    inverse = lax.rsqrt(squares / full_width + EPSILON)
    coupling = inverse**3 * (crossed / full_width)
    mix_grad = (inverse[:, None] * scaled_grad - mixed * coupling[:, None]).astype(jnp.bfloat16)
    assigned = expert_ids.reshape(-1)
    n_assign = assigned.shape[0]
    one_hot = (assigned[:, None] == jnp.arange(n_experts, dtype=jnp.int32)[None, :]).astype(
        jnp.int32
    )
    before = jnp.sum((jnp.cumsum(one_hot, axis=0) - one_hot) * one_hot, axis=1)
    slot_of = assigned * capacity + before
    slot_source = (
        jnp.full((n_experts * capacity,), n_assign, jnp.int32)
        .at[slot_of]
        .set(jnp.arange(n_assign, dtype=jnp.int32))
    )
    slot_token = slot_source // top_count
    weight_pad = jnp.concatenate([gate_weights.reshape(-1), jnp.zeros((1,), jnp.bfloat16)])
    send_weight = weight_pad[slot_source].reshape(n_experts, capacity)
    token_slice = lax.dynamic_slice_in_dim(tokens, lax.axis_index("tp") * col_width, col_width, 1)
    part_tokens, part_grad, recv_weight = (
        lax.all_to_all(
            pick_rows(token_slice, slot_token, n_experts, capacity),
            "ep",
            split_axis=0,
            concat_axis=0,
            tiled=True,
        ),
        lax.all_to_all(
            pick_rows(mix_grad, slot_token, n_experts, capacity),
            "ep",
            split_axis=0,
            concat_axis=0,
            tiled=True,
        ),
        lax.all_to_all(send_weight, "ep", split_axis=0, concat_axis=0, tiled=True),
    )
    recv_tokens, recv_grad = (
        lax.all_gather(part_tokens, "tp", axis=2, tiled=True),
        lax.all_gather(part_grad, "tp", axis=2, tiled=True),
    )
    layout = (ep_count, exp_local, capacity, full_width)
    inputs = recv_tokens.reshape(layout)
    cotangent = recv_grad.reshape(layout)
    scales = recv_weight.reshape(ep_count, exp_local, capacity, 1).astype(jnp.float32)
    gate_pre = jnp.einsum("secd,efd->secf", inputs, gate_w, preferred_element_type=jnp.float32)
    up_pre = jnp.einsum("secd,efd->secf", inputs, up_w, preferred_element_type=jnp.float32)
    hidden_grad = jnp.einsum(
        "secd,efd->secf", cotangent, down_w, preferred_element_type=jnp.float32
    )
    sigmoid = jax.nn.sigmoid(gate_pre)
    activated = gate_pre * sigmoid
    gate_part = jnp.sum(activated * up_pre * hidden_grad, axis=3)
    scaled_hidden = (scales * activated * up_pre).astype(jnp.bfloat16)
    down_grad = jnp.einsum(
        "secf,secd->efd", scaled_hidden, cotangent, preferred_element_type=jnp.float32
    )
    gate_delta = (
        scales * hidden_grad * up_pre * sigmoid * (1.0 + gate_pre * (1.0 - sigmoid))
    ).astype(jnp.bfloat16)
    up_delta = (scales * hidden_grad * activated).astype(jnp.bfloat16)
    gate_grad_w = jnp.einsum(
        "secf,secd->efd", gate_delta, inputs, preferred_element_type=jnp.float32
    )
    up_grad_w = jnp.einsum("secf,secd->efd", up_delta, inputs, preferred_element_type=jnp.float32)
    partial_value = jnp.einsum(
        "secf,efd->secd", gate_delta, gate_w, preferred_element_type=jnp.float32
    )
    partial_value = partial_value + jnp.einsum(
        "secf,efd->secd", up_delta, up_w, preferred_element_type=jnp.float32
    )
    gate_total = lax.psum(gate_part, "tp").astype(jnp.bfloat16)
    slot_grad = lax.psum_scatter(
        partial_value.astype(jnp.bfloat16), "tp", scatter_dimension=3, tiled=True
    )
    back_grad, back_gate = (
        lax.all_to_all(
            slot_grad.reshape(ep_count * exp_local, capacity, col_width),
            "ep",
            split_axis=0,
            concat_axis=0,
            tiled=True,
        ),
        lax.all_to_all(
            gate_total.reshape(ep_count * exp_local, capacity),
            "ep",
            split_axis=0,
            concat_axis=0,
            tiled=True,
        ),
    )
    token_rows = back_grad.reshape(n_experts * capacity, col_width)[slot_of].reshape(
        tok_count, top_count, col_width
    )
    token_grad = jnp.sum(token_rows.astype(jnp.float32), axis=1).astype(jnp.bfloat16)
    gate_grad = back_gate.reshape(-1)[slot_of].reshape(tok_count, top_count)
    return (token_grad, gate_grad, gate_grad_w, up_grad_w, down_grad)


def local(tokens, moe_out, out_grad, norm_gain, gate_weights, expert_ids, gate_w, up_w, down_w):
    tok_count, full_width = tokens.shape
    width = moe_out.shape[1]
    ep_count = lax.axis_size("ep")
    exp_local = gate_w.shape[0]
    if exp_local != 1 or lax.axis_size("tp") != 4 or ep_count % CORES:
        return general(
            tokens, moe_out, out_grad, norm_gain, gate_weights, expert_ids, gate_w, up_w, down_w
        )
    n_experts = ep_count * exp_local
    top_count = expert_ids.shape[1]
    expert_cap = 2 * tok_count * top_count // n_experts
    zs = ep_count // CORES
    cap = expert_cap if n_experts // GROUPS <= CORES else CORES * expert_cap
    slots = ep_count * cap

    chip_of = expert_ids // CORES
    chips = jnp.arange(zs, dtype=jnp.int32)
    named = chip_of[:, :, None] == chips
    member = jnp.any(named, axis=1)
    earlier = (
        jnp.arange(tok_count, dtype=jnp.int32)[:, None]
        > jnp.arange(tok_count, dtype=jnp.int32)[None, :]
    ).astype(BF16)
    rank = jnp.dot(earlier, member.astype(BF16), preferred_element_type=F32).astype(jnp.int32)
    slot_of = jnp.where(member, rank, -1)
    places_at = jnp.arange(cap, dtype=jnp.int32)
    perm = (
        (slot_of.T[:, None, :] == places_at[None, :, None]).astype(BF16).reshape(zs * cap, tok_count)
    )
    chosen = expert_ids[:, :, None] == jnp.arange(LANES, dtype=jnp.int32)
    wmat = jnp.sum(jnp.where(chosen, gate_weights[:, :, None].astype(F32), 0.0), axis=1).astype(BF16)

    n_send = 3 + 3 * (zs - 1) + zs + 2 * zs * 7
    inputs, cotangent, weights = pl.pallas_call(
        functools.partial(dispatch_kernel, zs, cap, width),
        out_shape=(
            jax.ShapeDtypeStruct((slots, full_width), BF16),
            jax.ShapeDtypeStruct((slots, full_width), BF16),
            jax.ShapeDtypeStruct((slots, LANES), BF16),
        ),
        in_specs=[VMEM_SPEC] * 6,
        out_specs=(VMEM_SPEC,) * 3,
        scratch_shapes=[
            pltpu.VMEM((zs * cap, width), BF16),
            pltpu.VMEM((zs * cap, width), BF16),
            pltpu.VMEM((zs * cap, LANES), BF16),
            pltpu.VMEM((4, 8, -(-tok_count // LANES) * LANES), F32),
            pltpu.SemaphoreType.DMA((n_send,)),
            pltpu.SemaphoreType.DMA((3,)),
            pltpu.SemaphoreType.DMA((2, zs)),
            pltpu.SemaphoreType.DMA((zs,)),
            pltpu.SemaphoreType.DMA((zs,)),
            pltpu.SemaphoreType.DMA((2, zs, 3)),
            pltpu.SemaphoreType.DMA((2, zs, 4)),
        ],
        compiler_params=pltpu.CompilerParams(
            collective_id=0, has_side_effects=True, vmem_limit_bytes=48 * 1024 * 1024
        ),
    )(tokens, moe_out, out_grad, norm_gain.reshape(1, width), perm, wmat)

    core = lax.axis_index("ep")
    lane = jnp.arange(LANES, dtype=jnp.int32)
    scales = jnp.sum(
        jnp.where(lane == core, weights.astype(F32), 0.0), axis=1, keepdims=True
    )
    w_gate, w_up, w_down = gate_w[0], up_w[0], down_w[0]

    def contract(a, b, dims):
        return lax.dot_general(a, b, (dims, ((), ())), preferred_element_type=F32)

    gate_pre = contract(inputs, w_gate, ((1,), (1,)))
    up_pre = contract(inputs, w_up, ((1,), (1,)))
    hidden_grad = contract(cotangent, w_down, ((1,), (1,)))
    sigmoid = jax.nn.sigmoid(gate_pre)
    activated = gate_pre * sigmoid
    gate_part = jnp.sum(activated * up_pre * hidden_grad, axis=1).reshape(ep_count, cap)
    gate_part = jnp.pad(gate_part, ((0, 0), (0, LANES - cap)))
    scaled_hidden = (scales * activated * up_pre).astype(BF16)
    gate_delta = (
        scales * hidden_grad * up_pre * sigmoid * (1.0 + gate_pre * (1.0 - sigmoid))
    ).astype(BF16)
    up_delta = (scales * hidden_grad * activated).astype(BF16)
    partial_value = (
        contract(gate_delta, w_gate, ((1,), (0,))) + contract(up_delta, w_up, ((1,), (0,)))
    ).astype(BF16)
    down_grad = contract(scaled_hidden, cotangent, ((0,), (0,)))[None]
    gate_grad_w = contract(gate_delta, inputs, ((0,), (0,)))[None]
    up_grad_w = contract(up_delta, inputs, ((0,), (0,)))[None]

    half = width // 2
    n_send = 4 + zs + 4 * zs + 2 * zs + 2 * (zs - 1)
    back, totals = pl.pallas_call(
        functools.partial(return_kernel, zs, cap, width),
        out_shape=(
            jax.ShapeDtypeStruct((zs * cap, width), BF16),
            jax.ShapeDtypeStruct((zs, CORES, ep_count, LANES), F32),
        ),
        in_specs=[VMEM_SPEC] * 2,
        out_specs=(VMEM_SPEC,) * 2,
        scratch_shapes=[
            pltpu.VMEM((zs, cap, full_width), BF16),
            pltpu.VMEM((zs, cap, full_width), BF16),
            pltpu.VMEM((zs, 2, 2, cap, half), BF16),
            pltpu.VMEM((zs, 2, cap, half), BF16),
            pltpu.VMEM((zs, 2, cap, half), BF16),
            pltpu.VMEM((zs, cap, width), BF16),
            pltpu.VMEM((4, CORES, ep_count, LANES), F32),
            pltpu.SemaphoreType.DMA((n_send,)),
            pltpu.SemaphoreType.DMA((zs,)),
            pltpu.SemaphoreType.DMA((zs, 2, 2)),
            pltpu.SemaphoreType.DMA((zs, 2)),
            pltpu.SemaphoreType.DMA((zs,)),
            pltpu.SemaphoreType.DMA((4,)),
            pltpu.SemaphoreType.DMA((zs,)),
        ],
        compiler_params=pltpu.CompilerParams(
            collective_id=1, has_side_effects=True, vmem_limit_bytes=48 * 1024 * 1024
        ),
    )(partial_value, gate_part)

    token_grad = contract(perm, back, ((0,), (0,))).astype(BF16)
    me = lax.axis_index("ep")
    mine = lax.dynamic_index_in_dim(totals, me, 2, keepdims=False)[:, :, :cap]
    mine = mine.astype(BF16).astype(F32)
    here = slot_of[:, :, None] == places_at
    parity = expert_ids % CORES
    columns = []
    for k in range(top_count):
        pick = jnp.where(
            (parity[:, k] == 0)[:, None, None], mine[:, 0][None], mine[:, 1][None]
        )
        keep = here & named[:, k][:, :, None]
        columns.append(jnp.sum(jnp.where(keep, pick, 0.0), axis=(1, 2)))
    gate_grad = jnp.stack(columns, axis=1).astype(BF16)
    return (token_grad, gate_grad, gate_grad_w, up_grad_w, down_grad)


def solution(mesh):
    in_specs = (
        P("ep", None),
        P("ep", "tp"),
        P("ep", "tp"),
        P("tp"),
        P("ep", None),
        P("ep", None),
        P("ep", "tp", None),
        P("ep", "tp", None),
        P("ep", "tp", None),
    )
    out_specs = (
        P("ep", "tp"),
        P("ep", None),
        P("ep", "tp", None),
        P("ep", "tp", None),
        P("ep", "tp", None),
    )
    return jax.shard_map(local, mesh=mesh, in_specs=in_specs, out_specs=out_specs, check_vma=False)
```

```python
import functools

import jax
import jax.numpy as jnp
from jax import lax
from jax.experimental import pallas as pl
from jax.experimental.pallas import tpu as pltpu
from jax.sharding import PartitionSpec as P

EPSILON = 0.25
GROUPS = 4
CORES = 2
LANES = 128
MESH = pl.DeviceIdType.MESH
VMEM_SPEC = pl.BlockSpec(memory_space=pltpu.VMEM)
F32 = jnp.float32
BF16 = jnp.bfloat16


def places(zs):
    ep = lax.axis_index("ep")
    tp = lax.axis_index("tp")
    z = ep // CORES
    core = ep % CORES
    near_x = tp + 1 - 2 * (tp % 2)
    near_y = (tp + 2) % 4
    diag = (near_x + 2) % 4
    return ep, tp, z, core, near_x, near_y, diag


def greet(zs):
    ep, tp, z, core, near_x, near_y, diag = places(zs)
    barrier = pltpu.get_barrier_semaphore()
    peers = [(z * CORES + 1 - core, tp), (ep, near_x), (ep, near_y), (ep, diag)]
    peers += [(((z + k) % zs) * CORES + core, tp) for k in range(1, zs)]
    for peer in peers:
        pl.semaphore_signal(barrier, inc=1, device_id=peer, device_id_type=MESH)
    pl.semaphore_wait(barrier, len(peers))


class Sender:
    def __init__(self, send_sem):
        self.send_sem, self.started = send_sem, []

    def __call__(self, src, dst, recv_sem, device):
        copy = pltpu.make_async_remote_copy(
            src_ref=src,
            dst_ref=dst,
            send_sem=self.send_sem.at[len(self.started)],
            recv_sem=recv_sem,
            device_id=device,
            device_id_type=MESH,
        )
        copy.start()
        self.started.append(copy)
        return copy

    def finish(self):
        for copy in self.started:
            copy.wait_send()


def route_kernel(
    zs, cap, width,
    tok_hbm, moe_hbm, grad_hbm, gain_ref, perm_ref, wmat_ref, wg_hbm, wu_hbm, wd_hbm,
    back_ref, total_ref, dwg_ref, dwu_ref, dwd_ref,
    tok_ref, moe_ref, grad_ref, wg_ref, wu_ref, wd_ref, x_ref, g_ref, w_ref,
    pack_x, pack_g, pack_w, stats, hid_ref, gd_ref, ud_ref,
    part_ref, comb, pin, first_in, second_out, second_in, final, gates,
    load_sem, send_sem, stat_sem, z_sem, w_sem, wp_sem, tp_sem, pair_sem,
    pin_sem, one_sem, two_sem, back_sem, gate_sem, gz_sem,
):
    ep, tp, z, core, near_x, near_y, diag = places(zs)
    n_tok = tok_ref.shape[0]
    full = x_ref.shape[1]
    partner = (z * CORES + 1 - core, tp)
    send = Sender(send_sem)
    half = width // 2

    def cols(at):
        return pl.ds(pl.multiple_of(at * width, width), width)

    def half_cols(at, which):
        return pl.ds(pl.multiple_of(at * width + which * half, half), half)

    def source(k):
        return (z - k + zs) % zs

    def rows(q, who=None):
        start = (q * CORES + (core if who is None else who)) * cap
        return pl.ds(pl.multiple_of(start, 16), cap)

    def chip_rows(q):
        return pl.ds(pl.multiple_of(q * cap, 16), cap)

    loads = [
        pltpu.make_async_copy(src, dst, load_sem.at[i])
        for i, (src, dst) in enumerate((
            (moe_hbm, moe_ref), (grad_hbm, grad_ref), (tok_hbm.at[:, cols(tp)], tok_ref),
            (wg_hbm, wg_ref), (wu_hbm, wu_ref), (wd_hbm, wd_ref),
        ))
    ]
    for load in loads:
        load.start()
    loads[0].wait()
    loads[1].wait()
    mixed = moe_ref[...].astype(F32)
    scaled = grad_ref[...].astype(F32) * gain_ref[...]
    squares = jnp.sum(mixed * mixed, axis=1, keepdims=True)
    crossed = jnp.sum(scaled * mixed, axis=1, keepdims=True)
    lane = lax.broadcasted_iota(jnp.int32, (n_tok, LANES), 1)
    both = jnp.where(lane == 0, squares, jnp.where(lane == 1, crossed, 0.0))
    tall = stats.shape[2]
    both = jnp.concatenate([both, jnp.zeros((tall - n_tok, LANES), F32)], axis=0)
    stats[0] = both.T[:8]
    greet(zs)
    got_stats = [
        send(stats.at[0], stats.at[1 + i], stat_sem.at[i], (ep, to))
        for i, to in enumerate((near_x, near_y, diag))
    ]

    loads[2].wait()
    perm = perm_ref[...]
    pack_x[...] = jnp.dot(perm, tok_ref[...], preferred_element_type=F32).astype(BF16)
    pack_w[...] = jnp.dot(perm, wmat_ref[...], preferred_element_type=F32).astype(BF16)
    x_ref[rows(z), cols(tp)] = pack_x[chip_rows(z), :]
    w_ref[rows(z), :] = pack_w[chip_rows(z), :]
    outs, packs = (x_ref, g_ref), (pack_x, pack_g)
    z_copies, w_copies = {}, {}

    def z_out(t):
        for k in range(1, zs):
            q = (z + k) % zs
            z_copies[t, k] = send(
                packs[t].at[chip_rows(q)],
                outs[t].at[rows(z), cols(tp)],
                z_sem.at[t, k],
                (q * CORES + core, tp),
            )

    z_out(0)
    tp_copies, pair_copies = {}, {}

    def to_pair(t, k, origin, at):
        block = outs[t].at[rows(source(k)), cols(at)]
        pair_copies[t, k, origin] = send(block, block, pair_sem.at[t, k, origin], partner)

    def arrive(t, k):
        if k:
            z_copies[t, k].wait_recv()
        block = outs[t].at[rows(source(k)), cols(tp)]
        tp_copies[t, k, 0] = send(block, block, tp_sem.at[t, k, 0], (ep, near_x))
        tp_copies[t, k, 1] = send(block, block, tp_sem.at[t, k, 1], (ep, near_y))
        to_pair(t, k, 0, tp)

    def relay(t, k):
        tp_copies[t, k, 0].wait_recv()
        tp_copies[t, k, 1].wait_recv()
        at, to = ((near_x, near_y), (near_y, near_x))[t]
        block = outs[t].at[rows(source(k)), cols(at)]
        tp_copies[t, k, 2] = send(block, block, tp_sem.at[t, k, 2], (ep, to))
        to_pair(t, k, 1, near_x)
        to_pair(t, k, 2, near_y)

    arrive(0, 0)
    for copy in got_stats:
        copy.wait_recv()
    total = stats[0] + stats[1] + stats[2] + stats[3]
    total = jnp.concatenate([total, jnp.zeros((LANES - 8, tall), F32)], axis=0).T[:n_tok]
    inverse = lax.rsqrt(total[:, 0:1] / full + EPSILON)
    coupling = inverse * inverse * inverse * (total[:, 1:2] / full)
    mix = (inverse * scaled - mixed * coupling).astype(BF16)
    pack_g[...] = jnp.dot(perm, mix, preferred_element_type=F32).astype(BF16)
    g_ref[rows(z), cols(tp)] = pack_g[chip_rows(z), :]
    z_out(1)
    for k in range(1, zs):
        q = (z + k) % zs
        w_copies[k] = send(
            pack_w.at[chip_rows(q)], w_ref.at[rows(z)], w_sem.at[k], (q * CORES + core, tp)
        )

    def last_part(k):
        for t in range(2):
            tp_copies[t, k, 2].wait_recv()
            to_pair(t, k, 3, diag)
        if k:
            w_copies[k].wait_recv()
        block = w_ref.at[rows(source(k))]
        pair_copies["w", k] = send(block, block, wp_sem.at[k], partner)

    nt = (((1,), (1,)), ((), ()))

    def compute(k):
        q = source(k)
        for t in range(2):
            for origin in range(4):
                pair_copies[t, k, origin].wait_recv()
        pair_copies["w", k].wait_recv()
        block = pl.ds(pl.multiple_of(q * (CORES * cap), 16), CORES * cap)
        x = x_ref[block, :]
        gate_pre = lax.dot_general(x, wg_ref[0], nt, preferred_element_type=F32)
        up_pre = lax.dot_general(x, wu_ref[0], nt, preferred_element_type=F32)
        hidden_grad = lax.dot_general(g_ref[block, :], wd_ref[0], nt, preferred_element_type=F32)
        lane = lax.broadcasted_iota(jnp.int32, (CORES * cap, LANES), 1)
        scales = jnp.sum(
            jnp.where(lane == ep, w_ref[block, :].astype(F32), 0.0), axis=1, keepdims=True
        )
        sigmoid = jax.nn.sigmoid(gate_pre)
        activated = gate_pre * sigmoid
        both = activated * up_pre
        gate_part = jnp.sum(both * hidden_grad, axis=1, keepdims=True)
        for who in range(CORES):
            tile = jnp.broadcast_to(gate_part[who * cap : (who + 1) * cap], (cap, LANES))
            tile = jnp.concatenate([tile, jnp.zeros((LANES - cap, LANES), F32)], axis=0).T
            gates[0, core, pl.ds(q * CORES + who, 1), :] = tile[0:1]
        weighted = scales * hidden_grad
        gate_delta = (weighted * up_pre * sigmoid * (1.0 + gate_pre * (1.0 - sigmoid))).astype(BF16)
        up_delta = (weighted * activated).astype(BF16)
        hid_ref[block, :] = (scales * both).astype(BF16)
        gd_ref[block, :] = gate_delta
        ud_ref[block, :] = up_delta

        @pl.loop(0, full // width)
        def _(at):
            columns = cols(at)
            value = jnp.dot(gd_ref[block, :], wg_ref[0, :, columns], preferred_element_type=F32)
            value += jnp.dot(ud_ref[block, :], wu_ref[0, :, columns], preferred_element_type=F32)
            part_ref[block, columns] = value.astype(BF16)

    def weight_grad(out_ref, delta_ref, rows_ref):
        flipped = delta_ref[...].T

        @pl.loop(0, full // half)
        def _(at):
            columns = pl.ds(pl.multiple_of(at * half, half), half)
            out_ref[0, :, columns] = jnp.dot(
                flipped, rows_ref[:, columns], preferred_element_type=F32
            )

    pin_copies, one, two, back = {}, {}, {}, {}

    def to_other_core(k):
        pin_copies[k] = send(
            part_ref.at[rows(source(k), 1 - core)], pin.at[k], pin_sem.at[k], partner
        )

    def stage_one(k):
        pin_copies[k].wait_recv()
        comb[k] = (part_ref[rows(source(k)), :].astype(F32) + pin[k].astype(F32)).astype(BF16)
        for which, near in enumerate((near_x, near_y)):
            for i, at in ((1, diag), (0, near)):
                one[k, which, i] = send(
                    comb.at[k, :, half_cols(at, which)],
                    first_in.at[k, which, i],
                    one_sem.at[k, which, i],
                    (ep, near),
                )

    def stage_two(k):
        for which, far in enumerate((near_y, near_x)):
            one[k, which, 1].wait_recv()
            second_out[k, which] = (
                comb[k, :, half_cols(far, which)].astype(F32) + first_in[k, which, 1].astype(F32)
            ).astype(BF16)
            two[k, which] = send(
                second_out.at[k, which], second_in.at[k, which], two_sem.at[k, which], (ep, far)
            )

    def stage_three(k):
        for which in range(2):
            one[k, which, 0].wait_recv()
            two[k, which].wait_recv()
            final[k, :, which * half : (which + 1) * half] = (
                comb[k, :, half_cols(tp, which)].astype(F32)
                + first_in[k, which, 0].astype(F32)
                + second_in[k, which].astype(F32)
            ).astype(BF16)
        if k:
            back[k] = send(
                final.at[k], back_ref.at[chip_rows(z)], back_sem.at[k],
                (source(k) * CORES + core, tp),
            )
        else:
            back_ref[chip_rows(z), :] = final[0]

    for step in range(zs + 3):
        for t in range(2):
            if step < zs:
                arrive(t, step) if (t, step) != (0, 0) else None
            if 0 <= step - 1 < zs:
                relay(t, step - 1)
        if 0 <= step - 2 < zs:
            last_part(step - 2)
        k = step - 3
        if k >= 0:
            if k == 0:
                for load in loads[3:]:
                    load.wait()
            compute(k)
            to_other_core(k)
            if k >= 1:
                stage_one(k - 1)
            if k >= 2:
                stage_two(k - 2)
            if k >= 3:
                stage_three(k - 3)

    last = zs - 1
    pair_gate = send(gates.at[0, core], gates.at[0, core], gate_sem.at[3], partner)
    stage_one(last)
    if last >= 1:
        stage_two(last - 1)
    pair_gate.wait_recv()
    gate_copies = [
        send(gates.at[0], gates.at[1 + i], gate_sem.at[i], (ep, to))
        for i, to in enumerate((near_x, near_y, diag))
    ]
    weight_grad(dwd_ref, hid_ref, g_ref)
    stage_two(last)
    for k in range(max(last - 2, 0), last):
        stage_three(k)
    for copy in gate_copies:
        copy.wait_recv()
    total_ref[z] = gates[0] + gates[1] + gates[2] + gates[3]
    gate_back = [
        send(total_ref.at[z], total_ref.at[z], gz_sem.at[k], (((z + k) % zs) * CORES + core, tp))
        for k in range(1, zs)
    ]
    weight_grad(dwg_ref, gd_ref, x_ref)
    stage_three(last)
    weight_grad(dwu_ref, ud_ref, x_ref)
    for copy in list(back.values()) + gate_back:
        copy.wait_recv()
    send.finish()


def pick_rows(matrix, slot_token, n_experts, capacity):
    padded = jnp.concatenate([matrix, jnp.zeros((1, matrix.shape[1]), matrix.dtype)], axis=0)
    return padded[slot_token].reshape(n_experts, capacity, matrix.shape[1])


def general(tokens, moe_out, out_grad, norm_gain, gate_weights, expert_ids, gate_w, up_w, down_w):
    tok_count = tokens.shape[0]
    full_width = tokens.shape[1]
    col_width = moe_out.shape[1]
    ep_count = lax.axis_size("ep")
    exp_local = gate_w.shape[0]
    n_experts = ep_count * exp_local
    top_count = expert_ids.shape[1]
    capacity = 2 * tok_count * top_count // n_experts
    mixed = moe_out.astype(jnp.float32)
    scaled_grad = out_grad.astype(jnp.float32) * norm_gain
    squares, crossed = lax.psum(
        (jnp.sum(mixed * mixed, axis=1), jnp.sum(scaled_grad * mixed, axis=1)), "tp"
    )
    inverse = lax.rsqrt(squares / full_width + EPSILON)
    coupling = inverse**3 * (crossed / full_width)
    mix_grad = (inverse[:, None] * scaled_grad - mixed * coupling[:, None]).astype(jnp.bfloat16)
    assigned = expert_ids.reshape(-1)
    n_assign = assigned.shape[0]
    one_hot = (assigned[:, None] == jnp.arange(n_experts, dtype=jnp.int32)[None, :]).astype(
        jnp.int32
    )
    before = jnp.sum((jnp.cumsum(one_hot, axis=0) - one_hot) * one_hot, axis=1)
    slot_of = assigned * capacity + before
    slot_source = (
        jnp.full((n_experts * capacity,), n_assign, jnp.int32)
        .at[slot_of]
        .set(jnp.arange(n_assign, dtype=jnp.int32))
    )
    slot_token = slot_source // top_count
    weight_pad = jnp.concatenate([gate_weights.reshape(-1), jnp.zeros((1,), jnp.bfloat16)])
    send_weight = weight_pad[slot_source].reshape(n_experts, capacity)
    token_slice = lax.dynamic_slice_in_dim(tokens, lax.axis_index("tp") * col_width, col_width, 1)
    part_tokens, part_grad, recv_weight = (
        lax.all_to_all(
            pick_rows(token_slice, slot_token, n_experts, capacity),
            "ep",
            split_axis=0,
            concat_axis=0,
            tiled=True,
        ),
        lax.all_to_all(
            pick_rows(mix_grad, slot_token, n_experts, capacity),
            "ep",
            split_axis=0,
            concat_axis=0,
            tiled=True,
        ),
        lax.all_to_all(send_weight, "ep", split_axis=0, concat_axis=0, tiled=True),
    )
    recv_tokens, recv_grad = (
        lax.all_gather(part_tokens, "tp", axis=2, tiled=True),
        lax.all_gather(part_grad, "tp", axis=2, tiled=True),
    )
    layout = (ep_count, exp_local, capacity, full_width)
    inputs = recv_tokens.reshape(layout)
    cotangent = recv_grad.reshape(layout)
    scales = recv_weight.reshape(ep_count, exp_local, capacity, 1).astype(jnp.float32)
    gate_pre = jnp.einsum("secd,efd->secf", inputs, gate_w, preferred_element_type=jnp.float32)
    up_pre = jnp.einsum("secd,efd->secf", inputs, up_w, preferred_element_type=jnp.float32)
    hidden_grad = jnp.einsum(
        "secd,efd->secf", cotangent, down_w, preferred_element_type=jnp.float32
    )
    sigmoid = jax.nn.sigmoid(gate_pre)
    activated = gate_pre * sigmoid
    gate_part = jnp.sum(activated * up_pre * hidden_grad, axis=3)
    scaled_hidden = (scales * activated * up_pre).astype(jnp.bfloat16)
    down_grad = jnp.einsum(
        "secf,secd->efd", scaled_hidden, cotangent, preferred_element_type=jnp.float32
    )
    gate_delta = (
        scales * hidden_grad * up_pre * sigmoid * (1.0 + gate_pre * (1.0 - sigmoid))
    ).astype(jnp.bfloat16)
    up_delta = (scales * hidden_grad * activated).astype(jnp.bfloat16)
    gate_grad_w = jnp.einsum(
        "secf,secd->efd", gate_delta, inputs, preferred_element_type=jnp.float32
    )
    up_grad_w = jnp.einsum("secf,secd->efd", up_delta, inputs, preferred_element_type=jnp.float32)
    partial_value = jnp.einsum(
        "secf,efd->secd", gate_delta, gate_w, preferred_element_type=jnp.float32
    )
    partial_value = partial_value + jnp.einsum(
        "secf,efd->secd", up_delta, up_w, preferred_element_type=jnp.float32
    )
    gate_total = lax.psum(gate_part, "tp").astype(jnp.bfloat16)
    slot_grad = lax.psum_scatter(
        partial_value.astype(jnp.bfloat16), "tp", scatter_dimension=3, tiled=True
    )
    back_grad, back_gate = (
        lax.all_to_all(
            slot_grad.reshape(ep_count * exp_local, capacity, col_width),
            "ep",
            split_axis=0,
            concat_axis=0,
            tiled=True,
        ),
        lax.all_to_all(
            gate_total.reshape(ep_count * exp_local, capacity),
            "ep",
            split_axis=0,
            concat_axis=0,
            tiled=True,
        ),
    )
    token_rows = back_grad.reshape(n_experts * capacity, col_width)[slot_of].reshape(
        tok_count, top_count, col_width
    )
    token_grad = jnp.sum(token_rows.astype(jnp.float32), axis=1).astype(jnp.bfloat16)
    gate_grad = back_gate.reshape(-1)[slot_of].reshape(tok_count, top_count)
    return (token_grad, gate_grad, gate_grad_w, up_grad_w, down_grad)


def local(tokens, moe_out, out_grad, norm_gain, gate_weights, expert_ids, gate_w, up_w, down_w):
    tok_count, full_width = tokens.shape
    width = moe_out.shape[1]
    ep_count = lax.axis_size("ep")
    exp_local = gate_w.shape[0]
    if exp_local != 1 or lax.axis_size("tp") != 4 or ep_count % CORES:
        return general(
            tokens, moe_out, out_grad, norm_gain, gate_weights, expert_ids, gate_w, up_w, down_w
        )
    n_experts = ep_count * exp_local
    top_count = expert_ids.shape[1]
    expert_cap = 2 * tok_count * top_count // n_experts
    zs = ep_count // CORES
    cap = expert_cap if n_experts // GROUPS <= CORES else CORES * expert_cap
    slots = ep_count * cap

    chip_of = expert_ids // CORES
    chips = jnp.arange(zs, dtype=jnp.int32)
    named = chip_of[:, :, None] == chips
    member = jnp.any(named, axis=1)
    earlier = (
        jnp.arange(tok_count, dtype=jnp.int32)[:, None]
        > jnp.arange(tok_count, dtype=jnp.int32)[None, :]
    ).astype(BF16)
    rank = jnp.dot(earlier, member.astype(BF16), preferred_element_type=F32).astype(jnp.int32)
    slot_of = jnp.where(member, rank, -1)
    places_at = jnp.arange(cap, dtype=jnp.int32)
    perm = (
        (slot_of.T[:, None, :] == places_at[None, :, None]).astype(BF16).reshape(zs * cap, tok_count)
    )
    chosen = expert_ids[:, :, None] == jnp.arange(LANES, dtype=jnp.int32)
    wmat = jnp.sum(jnp.where(chosen, gate_weights[:, :, None].astype(F32), 0.0), axis=1).astype(BF16)

    half = width // 2
    hidden = gate_w.shape[1]
    n_send = 3 + 3 * (zs - 1) + zs + 2 * zs * 7
    n_send += 4 + zs + 4 * zs + 2 * zs + 2 * (zs - 1)
    dw_shape = jax.ShapeDtypeStruct(gate_w.shape, F32)
    any_spec = pl.BlockSpec(memory_space=pl.ANY)
    sem = pltpu.SemaphoreType.DMA
    back, totals, gate_grad_w, up_grad_w, down_grad = pl.pallas_call(
        functools.partial(route_kernel, zs, cap, width),
        out_shape=(
            jax.ShapeDtypeStruct((zs * cap, width), BF16),
            jax.ShapeDtypeStruct((zs, CORES, ep_count, LANES), F32),
            dw_shape,
            dw_shape,
            dw_shape,
        ),
        in_specs=[any_spec] * 3 + [VMEM_SPEC] * 3 + [any_spec] * 3,
        out_specs=(VMEM_SPEC,) * 5,
        scratch_shapes=[
            pltpu.VMEM((tok_count, width), BF16),
            pltpu.VMEM((tok_count, width), BF16),
            pltpu.VMEM((tok_count, width), BF16),
            pltpu.VMEM(gate_w.shape, BF16),
            pltpu.VMEM(gate_w.shape, BF16),
            pltpu.VMEM(gate_w.shape, BF16),
            pltpu.VMEM((slots, full_width), BF16),
            pltpu.VMEM((slots, full_width), BF16),
            pltpu.VMEM((slots, LANES), BF16),
            pltpu.VMEM((zs * cap, width), BF16),
            pltpu.VMEM((zs * cap, width), BF16),
            pltpu.VMEM((zs * cap, LANES), BF16),
            pltpu.VMEM((4, 8, -(-tok_count // LANES) * LANES), F32),
            pltpu.VMEM((slots, hidden), BF16),
            pltpu.VMEM((slots, hidden), BF16),
            pltpu.VMEM((slots, hidden), BF16),
            pltpu.VMEM((slots, full_width), BF16),
            pltpu.VMEM((zs, cap, full_width), BF16),
            pltpu.VMEM((zs, cap, full_width), BF16),
            pltpu.VMEM((zs, 2, 2, cap, half), BF16),
            pltpu.VMEM((zs, 2, cap, half), BF16),
            pltpu.VMEM((zs, 2, cap, half), BF16),
            pltpu.VMEM((zs, cap, width), BF16),
            pltpu.VMEM((4, CORES, ep_count, LANES), F32),
            sem((6,)),
            sem((n_send,)),
            sem((3,)),
            sem((2, zs)),
            sem((zs,)),
            sem((zs,)),
            sem((2, zs, 3)),
            sem((2, zs, 4)),
            sem((zs,)),
            sem((zs, 2, 2)),
            sem((zs, 2)),
            sem((zs,)),
            sem((4,)),
            sem((zs,)),
        ],
        compiler_params=pltpu.CompilerParams(
            collective_id=0, has_side_effects=True, vmem_limit_bytes=60 * 1024 * 1024
        ),
    )(
        tokens, moe_out, out_grad, norm_gain.reshape(1, width), perm, wmat, gate_w, up_w, down_w
    )

    token_grad = lax.dot_general(
        perm, back, (((0,), (0,)), ((), ())), preferred_element_type=F32
    ).astype(BF16)
    me = lax.axis_index("ep")
    mine = lax.dynamic_index_in_dim(totals, me, 2, keepdims=False)[:, :, :cap]
    mine = mine.astype(BF16).astype(F32)
    here = slot_of[:, :, None] == places_at
    parity = expert_ids % CORES
    columns = []
    for k in range(top_count):
        pick = jnp.where(
            (parity[:, k] == 0)[:, None, None], mine[:, 0][None], mine[:, 1][None]
        )
        keep = here & named[:, k][:, :, None]
        columns.append(jnp.sum(jnp.where(keep, pick, 0.0), axis=(1, 2)))
    gate_grad = jnp.stack(columns, axis=1).astype(BF16)
    return (token_grad, gate_grad, gate_grad_w, up_grad_w, down_grad)


def solution(mesh):
    in_specs = (
        P("ep", None),
        P("ep", "tp"),
        P("ep", "tp"),
        P("tp"),
        P("ep", None),
        P("ep", None),
        P("ep", "tp", None),
        P("ep", "tp", None),
        P("ep", "tp", None),
    )
    out_specs = (
        P("ep", "tp"),
        P("ep", None),
        P("ep", "tp", None),
        P("ep", "tp", None),
        P("ep", "tp", None),
    )
    return jax.shard_map(local, mesh=mesh, in_specs=in_specs, out_specs=out_specs, check_vma=False)
```

```python
import functools

import jax
import jax.numpy as jnp
from jax import lax
from jax.experimental import pallas as pl
from jax.experimental.pallas import tpu as pltpu
from jax.sharding import PartitionSpec as P

EPSILON = 0.25
GROUPS = 4
CORES = 2
LANES = 128
MESH = pl.DeviceIdType.MESH
VMEM_SPEC = pl.BlockSpec(memory_space=pltpu.VMEM)
F32 = jnp.float32
BF16 = jnp.bfloat16


def places(zs):
    ep = lax.axis_index("ep")
    tp = lax.axis_index("tp")
    z = ep // CORES
    core = ep % CORES
    near_x = tp + 1 - 2 * (tp % 2)
    near_y = (tp + 2) % 4
    diag = (near_x + 2) % 4
    return ep, tp, z, core, near_x, near_y, diag


def greet(zs):
    ep, tp, z, core, near_x, near_y, diag = places(zs)
    barrier = pltpu.get_barrier_semaphore()
    peers = [(z * CORES + 1 - core, tp), (ep, near_x), (ep, near_y), (ep, diag)]
    peers += [(((z + k) % zs) * CORES + core, tp) for k in range(1, zs)]
    for peer in peers:
        pl.semaphore_signal(barrier, inc=1, device_id=peer, device_id_type=MESH)
    pl.semaphore_wait(barrier, len(peers))


class Sender:
    def __init__(self, send_sem):
        self.send_sem, self.started = send_sem, []

    def __call__(self, src, dst, recv_sem, device):
        copy = pltpu.make_async_remote_copy(
            src_ref=src,
            dst_ref=dst,
            send_sem=self.send_sem.at[len(self.started)],
            recv_sem=recv_sem,
            device_id=device,
            device_id_type=MESH,
        )
        copy.start()
        self.started.append(copy)
        return copy

    def finish(self):
        for copy in self.started:
            copy.wait_send()


def route_kernel(
    zs, cap, width,
    tok_hbm, moe_hbm, grad_hbm, gain_ref, perm_ref, wmat_ref, wg_hbm, wu_hbm, wd_hbm,
    back_ref, total_ref, dwg_ref, dwu_ref, dwd_ref,
    tok_ref, moe_ref, grad_ref, wg_ref, wu_ref, wd_ref, x_ref, g_ref, w_ref,
    pack_x, pack_g, pack_w, stats, hid_ref, gd_ref, ud_ref,
    part_ref, comb, pin, first_in, second_out, second_in, final, gates,
    load_sem, send_sem, stat_sem, z_sem, w_sem, wp_sem, tp_sem, pair_sem,
    pin_sem, one_sem, two_sem, back_sem, gate_sem, gz_sem,
):
    ep, tp, z, core, near_x, near_y, diag = places(zs)
    n_tok = tok_ref.shape[0]
    full = x_ref.shape[1]
    partner = (z * CORES + 1 - core, tp)
    send = Sender(send_sem)
    half = width // 2

    def cols(at):
        return pl.ds(pl.multiple_of(at * width, width), width)

    def half_cols(at, which):
        return pl.ds(pl.multiple_of(at * width + which * half, half), half)

    def source(k):
        return (z - k + zs) % zs

    def rows(q, who=None):
        start = (q * CORES + (core if who is None else who)) * cap
        return pl.ds(pl.multiple_of(start, 16), cap)

    def chip_rows(q):
        return pl.ds(pl.multiple_of(q * cap, 16), cap)

    loads = [
        pltpu.make_async_copy(src, dst, load_sem.at[i])
        for i, (src, dst) in enumerate((
            (moe_hbm, moe_ref), (grad_hbm, grad_ref), (tok_hbm.at[:, cols(tp)], tok_ref),
            (wg_hbm, wg_ref), (wu_hbm, wu_ref), (wd_hbm, wd_ref),
        ))
    ]
    for load in loads:
        load.start()
    loads[0].wait()
    loads[1].wait()
    mixed = moe_ref[...].astype(F32)
    scaled = grad_ref[...].astype(F32) * gain_ref[...]
    squares = jnp.sum(mixed * mixed, axis=1, keepdims=True)
    crossed = jnp.sum(scaled * mixed, axis=1, keepdims=True)
    lane = lax.broadcasted_iota(jnp.int32, (n_tok, LANES), 1)
    both = jnp.where(lane == 0, squares, jnp.where(lane == 1, crossed, 0.0))
    tall = stats.shape[2]
    both = jnp.concatenate([both, jnp.zeros((tall - n_tok, LANES), F32)], axis=0)
    stats[0] = both.T[:8]
    greet(zs)
    got_stats = [
        send(stats.at[0], stats.at[1 + i], stat_sem.at[i], (ep, to))
        for i, to in enumerate((near_x, near_y, diag))
    ]

    loads[2].wait()
    perm = perm_ref[...]
    pack_x[...] = jnp.dot(perm, tok_ref[...], preferred_element_type=F32).astype(BF16)
    pack_w[...] = jnp.dot(perm, wmat_ref[...], preferred_element_type=F32).astype(BF16)
    x_ref[rows(z), cols(tp)] = pack_x[chip_rows(z), :]
    w_ref[rows(z), :] = pack_w[chip_rows(z), :]
    outs, packs = (x_ref, g_ref), (pack_x, pack_g)
    z_copies, w_copies = {}, {}

    def z_out(t):
        for k in range(1, zs):
            q = (z + k) % zs
            z_copies[t, k] = send(
                packs[t].at[chip_rows(q)],
                outs[t].at[rows(z), cols(tp)],
                z_sem.at[t, k],
                (q * CORES + core, tp),
            )

    z_out(0)
    tp_copies, pair_copies = {}, {}

    def to_pair(t, k, origin, at):
        block = outs[t].at[rows(source(k)), cols(at)]
        pair_copies[t, k, origin] = send(block, block, pair_sem.at[t, k, origin], partner)

    def arrive(t, k):
        if k:
            z_copies[t, k].wait_recv()
        block = outs[t].at[rows(source(k)), cols(tp)]
        tp_copies[t, k, 0] = send(block, block, tp_sem.at[t, k, 0], (ep, near_x))
        tp_copies[t, k, 1] = send(block, block, tp_sem.at[t, k, 1], (ep, near_y))
        to_pair(t, k, 0, tp)

    def relay(t, k):
        tp_copies[t, k, 0].wait_recv()
        tp_copies[t, k, 1].wait_recv()
        at, to = ((near_x, near_y), (near_y, near_x))[t]
        block = outs[t].at[rows(source(k)), cols(at)]
        tp_copies[t, k, 2] = send(block, block, tp_sem.at[t, k, 2], (ep, to))
        to_pair(t, k, 1, near_x)
        to_pair(t, k, 2, near_y)

    arrive(0, 0)
    for copy in got_stats:
        copy.wait_recv()
    total = stats[0] + stats[1] + stats[2] + stats[3]
    total = jnp.concatenate([total, jnp.zeros((LANES - 8, tall), F32)], axis=0).T[:n_tok]
    inverse = lax.rsqrt(total[:, 0:1] / full + EPSILON)
    coupling = inverse * inverse * inverse * (total[:, 1:2] / full)
    mix = (inverse * scaled - mixed * coupling).astype(BF16)
    pack_g[...] = jnp.dot(perm, mix, preferred_element_type=F32).astype(BF16)
    g_ref[rows(z), cols(tp)] = pack_g[chip_rows(z), :]
    z_out(1)
    for k in range(1, zs):
        q = (z + k) % zs
        w_copies[k] = send(
            pack_w.at[chip_rows(q)], w_ref.at[rows(z)], w_sem.at[k], (q * CORES + core, tp)
        )

    def last_part(k):
        for t in range(2):
            tp_copies[t, k, 2].wait_recv()
            to_pair(t, k, 3, diag)
        if k:
            w_copies[k].wait_recv()
        block = w_ref.at[rows(source(k))]
        pair_copies["w", k] = send(block, block, wp_sem.at[k], partner)

    nt = (((1,), (1,)), ((), ()))

    def compute(k):
        q = source(k)
        for t in range(2):
            for origin in range(4):
                pair_copies[t, k, origin].wait_recv()
        pair_copies["w", k].wait_recv()
        block = pl.ds(pl.multiple_of(q * (CORES * cap), 16), CORES * cap)
        x = x_ref[block, :]
        gate_pre = lax.dot_general(x, wg_ref[0], nt, preferred_element_type=F32)
        up_pre = lax.dot_general(x, wu_ref[0], nt, preferred_element_type=F32)
        hidden_grad = lax.dot_general(g_ref[block, :], wd_ref[0], nt, preferred_element_type=F32)
        lane = lax.broadcasted_iota(jnp.int32, (CORES * cap, LANES), 1)
        scales = jnp.sum(
            jnp.where(lane == ep, w_ref[block, :].astype(F32), 0.0), axis=1, keepdims=True
        )
        sigmoid = jax.nn.sigmoid(gate_pre)
        activated = gate_pre * sigmoid
        both = activated * up_pre
        gate_part = jnp.sum(both * hidden_grad, axis=1, keepdims=True)
        for who in range(CORES):
            tile = jnp.broadcast_to(gate_part[who * cap : (who + 1) * cap], (cap, LANES))
            tile = jnp.concatenate([tile, jnp.zeros((LANES - cap, LANES), F32)], axis=0).T
            gates[0, core, pl.ds(q * CORES + who, 1), :] = tile[0:1]
        weighted = scales * hidden_grad
        gate_delta = (weighted * up_pre * sigmoid * (1.0 + gate_pre * (1.0 - sigmoid))).astype(BF16)
        up_delta = (weighted * activated).astype(BF16)
        hid_ref[block, :] = (scales * both).astype(BF16)
        gd_ref[block, :] = gate_delta
        ud_ref[block, :] = up_delta

    def input_grad(k):
        block = pl.ds(pl.multiple_of(source(k) * (CORES * cap), 16), CORES * cap)

        @pl.loop(0, full // width)
        def _(at):
            columns = cols(at)
            value = jnp.dot(gd_ref[block, :], wg_ref[0, :, columns], preferred_element_type=F32)
            value += jnp.dot(ud_ref[block, :], wu_ref[0, :, columns], preferred_element_type=F32)
            part_ref[block, columns] = value.astype(BF16)

    def weight_grad(out_ref, delta_ref, rows_ref):
        flipped = delta_ref[...].T

        @pl.loop(0, full // half)
        def _(at):
            columns = pl.ds(pl.multiple_of(at * half, half), half)
            out_ref[0, :, columns] = jnp.dot(
                flipped, rows_ref[:, columns], preferred_element_type=F32
            )

    pin_copies, one, two, back = {}, {}, {}, {}

    def to_other_core(k):
        pin_copies[k] = send(
            part_ref.at[rows(source(k), 1 - core)], pin.at[k], pin_sem.at[k], partner
        )

    def stage_one(k):
        pin_copies[k].wait_recv()
        comb[k] = (part_ref[rows(source(k)), :].astype(F32) + pin[k].astype(F32)).astype(BF16)
        for which, near in enumerate((near_x, near_y)):
            for i, at in ((1, diag), (0, near)):
                one[k, which, i] = send(
                    comb.at[k, :, half_cols(at, which)],
                    first_in.at[k, which, i],
                    one_sem.at[k, which, i],
                    (ep, near),
                )

    def stage_two(k):
        for which, far in enumerate((near_y, near_x)):
            one[k, which, 1].wait_recv()
            second_out[k, which] = (
                comb[k, :, half_cols(far, which)].astype(F32) + first_in[k, which, 1].astype(F32)
            ).astype(BF16)
            two[k, which] = send(
                second_out.at[k, which], second_in.at[k, which], two_sem.at[k, which], (ep, far)
            )

    def stage_three(k):
        for which in range(2):
            one[k, which, 0].wait_recv()
            two[k, which].wait_recv()
            final[k, :, which * half : (which + 1) * half] = (
                comb[k, :, half_cols(tp, which)].astype(F32)
                + first_in[k, which, 0].astype(F32)
                + second_in[k, which].astype(F32)
            ).astype(BF16)
        if k:
            back[k] = send(
                final.at[k], back_ref.at[chip_rows(z)], back_sem.at[k],
                (source(k) * CORES + core, tp),
            )
        else:
            back_ref[chip_rows(z), :] = final[0]

    last = zs - 1
    for step in range(zs + 2):
        if 0 <= step - 2:
            last_part(step - 2)
        for t in range(2):
            if step < zs:
                arrive(t, step) if (t, step) != (0, 0) else None
            if 0 <= step - 1 < zs:
                relay(t, step - 1)
        k = step - 2
        if k >= 0:
            if k == 0:
                for load in loads[3:]:
                    load.wait()
            compute(k)
            if k >= 1:
                stage_one(k - 1)
            if k >= 2:
                stage_three(k - 2)
            input_grad(k)
            to_other_core(k)
            if k >= 1:
                stage_two(k - 1)

    pair_gate = send(gates.at[0, core], gates.at[0, core], gate_sem.at[3], partner)
    weight_grad(dwd_ref, hid_ref, g_ref)
    stage_one(last)
    if last >= 1:
        stage_three(last - 1)
    pair_gate.wait_recv()
    gate_copies = [
        send(gates.at[0], gates.at[1 + i], gate_sem.at[i], (ep, to))
        for i, to in enumerate((near_x, near_y, diag))
    ]
    weight_grad(dwg_ref, gd_ref, x_ref)
    stage_two(last)
    for copy in gate_copies:
        copy.wait_recv()
    total_ref[z] = gates[0] + gates[1] + gates[2] + gates[3]
    gate_back = [
        send(total_ref.at[z], total_ref.at[z], gz_sem.at[k], (((z + k) % zs) * CORES + core, tp))
        for k in range(1, zs)
    ]
    weight_grad(dwu_ref, ud_ref, x_ref)
    stage_three(last)
    for copy in list(back.values()) + gate_back:
        copy.wait_recv()
    send.finish()


def pick_rows(matrix, slot_token, n_experts, capacity):
    padded = jnp.concatenate([matrix, jnp.zeros((1, matrix.shape[1]), matrix.dtype)], axis=0)
    return padded[slot_token].reshape(n_experts, capacity, matrix.shape[1])


def general(tokens, moe_out, out_grad, norm_gain, gate_weights, expert_ids, gate_w, up_w, down_w):
    tok_count = tokens.shape[0]
    full_width = tokens.shape[1]
    col_width = moe_out.shape[1]
    ep_count = lax.axis_size("ep")
    exp_local = gate_w.shape[0]
    n_experts = ep_count * exp_local
    top_count = expert_ids.shape[1]
    capacity = 2 * tok_count * top_count // n_experts
    mixed = moe_out.astype(jnp.float32)
    scaled_grad = out_grad.astype(jnp.float32) * norm_gain
    squares, crossed = lax.psum(
        (jnp.sum(mixed * mixed, axis=1), jnp.sum(scaled_grad * mixed, axis=1)), "tp"
    )
    inverse = lax.rsqrt(squares / full_width + EPSILON)
    coupling = inverse**3 * (crossed / full_width)
    mix_grad = (inverse[:, None] * scaled_grad - mixed * coupling[:, None]).astype(jnp.bfloat16)
    assigned = expert_ids.reshape(-1)
    n_assign = assigned.shape[0]
    one_hot = (assigned[:, None] == jnp.arange(n_experts, dtype=jnp.int32)[None, :]).astype(
        jnp.int32
    )
    before = jnp.sum((jnp.cumsum(one_hot, axis=0) - one_hot) * one_hot, axis=1)
    slot_of = assigned * capacity + before
    slot_source = (
        jnp.full((n_experts * capacity,), n_assign, jnp.int32)
        .at[slot_of]
        .set(jnp.arange(n_assign, dtype=jnp.int32))
    )
    slot_token = slot_source // top_count
    weight_pad = jnp.concatenate([gate_weights.reshape(-1), jnp.zeros((1,), jnp.bfloat16)])
    send_weight = weight_pad[slot_source].reshape(n_experts, capacity)
    token_slice = lax.dynamic_slice_in_dim(tokens, lax.axis_index("tp") * col_width, col_width, 1)
    part_tokens, part_grad, recv_weight = (
        lax.all_to_all(
            pick_rows(token_slice, slot_token, n_experts, capacity),
            "ep",
            split_axis=0,
            concat_axis=0,
            tiled=True,
        ),
        lax.all_to_all(
            pick_rows(mix_grad, slot_token, n_experts, capacity),
            "ep",
            split_axis=0,
            concat_axis=0,
            tiled=True,
        ),
        lax.all_to_all(send_weight, "ep", split_axis=0, concat_axis=0, tiled=True),
    )
    recv_tokens, recv_grad = (
        lax.all_gather(part_tokens, "tp", axis=2, tiled=True),
        lax.all_gather(part_grad, "tp", axis=2, tiled=True),
    )
    layout = (ep_count, exp_local, capacity, full_width)
    inputs = recv_tokens.reshape(layout)
    cotangent = recv_grad.reshape(layout)
    scales = recv_weight.reshape(ep_count, exp_local, capacity, 1).astype(jnp.float32)
    gate_pre = jnp.einsum("secd,efd->secf", inputs, gate_w, preferred_element_type=jnp.float32)
    up_pre = jnp.einsum("secd,efd->secf", inputs, up_w, preferred_element_type=jnp.float32)
    hidden_grad = jnp.einsum(
        "secd,efd->secf", cotangent, down_w, preferred_element_type=jnp.float32
    )
    sigmoid = jax.nn.sigmoid(gate_pre)
    activated = gate_pre * sigmoid
    gate_part = jnp.sum(activated * up_pre * hidden_grad, axis=3)
    scaled_hidden = (scales * activated * up_pre).astype(jnp.bfloat16)
    down_grad = jnp.einsum(
        "secf,secd->efd", scaled_hidden, cotangent, preferred_element_type=jnp.float32
    )
    gate_delta = (
        scales * hidden_grad * up_pre * sigmoid * (1.0 + gate_pre * (1.0 - sigmoid))
    ).astype(jnp.bfloat16)
    up_delta = (scales * hidden_grad * activated).astype(jnp.bfloat16)
    gate_grad_w = jnp.einsum(
        "secf,secd->efd", gate_delta, inputs, preferred_element_type=jnp.float32
    )
    up_grad_w = jnp.einsum("secf,secd->efd", up_delta, inputs, preferred_element_type=jnp.float32)
    partial_value = jnp.einsum(
        "secf,efd->secd", gate_delta, gate_w, preferred_element_type=jnp.float32
    )
    partial_value = partial_value + jnp.einsum(
        "secf,efd->secd", up_delta, up_w, preferred_element_type=jnp.float32
    )
    gate_total = lax.psum(gate_part, "tp").astype(jnp.bfloat16)
    slot_grad = lax.psum_scatter(
        partial_value.astype(jnp.bfloat16), "tp", scatter_dimension=3, tiled=True
    )
    back_grad, back_gate = (
        lax.all_to_all(
            slot_grad.reshape(ep_count * exp_local, capacity, col_width),
            "ep",
            split_axis=0,
            concat_axis=0,
            tiled=True,
        ),
        lax.all_to_all(
            gate_total.reshape(ep_count * exp_local, capacity),
            "ep",
            split_axis=0,
            concat_axis=0,
            tiled=True,
        ),
    )
    token_rows = back_grad.reshape(n_experts * capacity, col_width)[slot_of].reshape(
        tok_count, top_count, col_width
    )
    token_grad = jnp.sum(token_rows.astype(jnp.float32), axis=1).astype(jnp.bfloat16)
    gate_grad = back_gate.reshape(-1)[slot_of].reshape(tok_count, top_count)
    return (token_grad, gate_grad, gate_grad_w, up_grad_w, down_grad)


def local(tokens, moe_out, out_grad, norm_gain, gate_weights, expert_ids, gate_w, up_w, down_w):
    tok_count, full_width = tokens.shape
    width = moe_out.shape[1]
    ep_count = lax.axis_size("ep")
    exp_local = gate_w.shape[0]
    if exp_local != 1 or lax.axis_size("tp") != 4 or ep_count % CORES:
        return general(
            tokens, moe_out, out_grad, norm_gain, gate_weights, expert_ids, gate_w, up_w, down_w
        )
    n_experts = ep_count * exp_local
    top_count = expert_ids.shape[1]
    expert_cap = 2 * tok_count * top_count // n_experts
    zs = ep_count // CORES
    cap = expert_cap if n_experts // GROUPS <= CORES else CORES * expert_cap
    slots = ep_count * cap

    chip_of = expert_ids // CORES
    chips = jnp.arange(zs, dtype=jnp.int32)
    named = chip_of[:, :, None] == chips
    member = jnp.any(named, axis=1)
    earlier = (
        jnp.arange(tok_count, dtype=jnp.int32)[:, None]
        > jnp.arange(tok_count, dtype=jnp.int32)[None, :]
    ).astype(BF16)
    rank = jnp.dot(earlier, member.astype(BF16), preferred_element_type=F32).astype(jnp.int32)
    slot_of = jnp.where(member, rank, -1)
    places_at = jnp.arange(cap, dtype=jnp.int32)
    perm = (
        (slot_of.T[:, None, :] == places_at[None, :, None]).astype(BF16).reshape(zs * cap, tok_count)
    )
    chosen = expert_ids[:, :, None] == jnp.arange(LANES, dtype=jnp.int32)
    wmat = jnp.sum(jnp.where(chosen, gate_weights[:, :, None].astype(F32), 0.0), axis=1).astype(BF16)

    half = width // 2
    hidden = gate_w.shape[1]
    n_send = 3 + 3 * (zs - 1) + zs + 2 * zs * 7
    n_send += 4 + zs + 4 * zs + 2 * zs + 2 * (zs - 1)
    dw_shape = jax.ShapeDtypeStruct(gate_w.shape, F32)
    any_spec = pl.BlockSpec(memory_space=pltpu.HBM)
    sem = pltpu.SemaphoreType.DMA
    back, totals, gate_grad_w, up_grad_w, down_grad = pl.pallas_call(
        functools.partial(route_kernel, zs, cap, width),
        out_shape=(
            jax.ShapeDtypeStruct((zs * cap, width), BF16),
            jax.ShapeDtypeStruct((zs, CORES, ep_count, LANES), F32),
            dw_shape,
            dw_shape,
            dw_shape,
        ),
        in_specs=[any_spec] * 3 + [VMEM_SPEC] * 3 + [any_spec] * 3,
        out_specs=(VMEM_SPEC,) * 5,
        scratch_shapes=[
            pltpu.VMEM((tok_count, width), BF16),
            pltpu.VMEM((tok_count, width), BF16),
            pltpu.VMEM((tok_count, width), BF16),
            pltpu.VMEM(gate_w.shape, BF16),
            pltpu.VMEM(gate_w.shape, BF16),
            pltpu.VMEM(gate_w.shape, BF16),
            pltpu.VMEM((slots, full_width), BF16),
            pltpu.VMEM((slots, full_width), BF16),
            pltpu.VMEM((slots, LANES), BF16),
            pltpu.VMEM((zs * cap, width), BF16),
            pltpu.VMEM((zs * cap, width), BF16),
            pltpu.VMEM((zs * cap, LANES), BF16),
            pltpu.VMEM((4, 8, -(-tok_count // LANES) * LANES), F32),
            pltpu.VMEM((slots, hidden), BF16),
            pltpu.VMEM((slots, hidden), BF16),
            pltpu.VMEM((slots, hidden), BF16),
            pltpu.VMEM((slots, full_width), BF16),
            pltpu.VMEM((zs, cap, full_width), BF16),
            pltpu.VMEM((zs, cap, full_width), BF16),
            pltpu.VMEM((zs, 2, 2, cap, half), BF16),
            pltpu.VMEM((zs, 2, cap, half), BF16),
            pltpu.VMEM((zs, 2, cap, half), BF16),
            pltpu.VMEM((zs, cap, width), BF16),
            pltpu.VMEM((4, CORES, ep_count, LANES), F32),
            sem((6,)),
            sem((n_send,)),
            sem((3,)),
            sem((2, zs)),
            sem((zs,)),
            sem((zs,)),
            sem((2, zs, 3)),
            sem((2, zs, 4)),
            sem((zs,)),
            sem((zs, 2, 2)),
            sem((zs, 2)),
            sem((zs,)),
            sem((4,)),
            sem((zs,)),
        ],
        compiler_params=pltpu.CompilerParams(
            collective_id=0, has_side_effects=True, vmem_limit_bytes=36 * 1024 * 1024
        ),
    )(
        *(pltpu.with_memory_space_constraint(a, pltpu.HBM) for a in (tokens, moe_out, out_grad)),
        norm_gain.reshape(1, width),
        perm,
        wmat,
        *(pltpu.with_memory_space_constraint(a, pltpu.HBM) for a in (gate_w, up_w, down_w)),
    )

    token_grad = lax.dot_general(
        perm, back, (((0,), (0,)), ((), ())), preferred_element_type=F32
    ).astype(BF16)
    me = lax.axis_index("ep")
    mine = lax.dynamic_index_in_dim(totals, me, 2, keepdims=False)[:, :, :cap]
    mine = mine.astype(BF16).astype(F32)
    here = slot_of[:, :, None] == places_at
    parity = expert_ids % CORES
    columns = []
    for k in range(top_count):
        pick = jnp.where(
            (parity[:, k] == 0)[:, None, None], mine[:, 0][None], mine[:, 1][None]
        )
        keep = here & named[:, k][:, :, None]
        columns.append(jnp.sum(jnp.where(keep, pick, 0.0), axis=(1, 2)))
    gate_grad = jnp.stack(columns, axis=1).astype(BF16)
    return (token_grad, gate_grad, gate_grad_w, up_grad_w, down_grad)


def solution(mesh):
    in_specs = (
        P("ep", None),
        P("ep", "tp"),
        P("ep", "tp"),
        P("tp"),
        P("ep", None),
        P("ep", None),
        P("ep", "tp", None),
        P("ep", "tp", None),
        P("ep", "tp", None),
    )
    out_specs = (
        P("ep", "tp"),
        P("ep", None),
        P("ep", "tp", None),
        P("ep", "tp", None),
        P("ep", "tp", None),
    )
    return jax.shard_map(local, mesh=mesh, in_specs=in_specs, out_specs=out_specs, check_vma=False)
```
